512 devices in a mesh: grp: 2 (over y), ep: 16 (over z), tp: 16 (over x, core).
Axes of the slice: x: 8, y: 2, z: 16, core: 2. Of those that a mesh axis runs over, the one named last changes fastest.
The devices are a block of a 8x16x16 slice.
Arguments:
- queries: bfloat16 [65536, 1024], P(('grp', 'ep'), 'tp'), parts along dimension 0, may hold values from -6 to 6
- key_vectors: bfloat16 [65536, 1024], P(('grp', 'ep'), 'tp'), parts along dimension 0, may hold values from -6 to 6
- value_vectors: bfloat16 [65536, 1024], P(('grp', 'ep'), 'tp'), parts along dimension 0, may hold values from -6 to 6
- input_gate: float32 [65536, 16], P(('grp', 'ep'), 'tp'), parts along dimension 0, may hold values from -6 to 320
- forget_gate: float32 [65536, 16], P(('grp', 'ep'), 'tp'), parts along dimension 0, may hold values from 0 to 15
- head_gain: float32 [1024], P('tp'), may hold values from 0.1 to 1.9
- out_weight: bfloat16 [1024, 2048], P(None, 'tp'), may hold values from -0.1875 to 0.1875
- expert_input: bfloat16 [4096, 2048], P(('grp', 'ep')), parts along dimension 0, may hold values from -6 to 6
- norm_gain: float32 [2048], replicated, may hold values from 0.1 to 1.9
- routes: int32 [4096, 2], P(('grp', 'ep')), parts along dimension 0, may hold values from 0 to 15, all different within a row; in each aligned block of 128 rows (0 to 127, 128 to 255, ...) at most 20 rows name the same one
- route_weight: float32 [4096, 2], P(('grp', 'ep')), parts along dimension 0, may hold values from 0.25 to 1
- gate_weight: bfloat16 [16, 2048, 3584], P('ep', None, 'tp'), may hold values from -0.125 to 0.125
- up_weight: bfloat16 [16, 2048, 3584], P('ep', None, 'tp'), may hold values from -0.125 to 0.125
- down_weight: bfloat16 [16, 3584, 2048], P('ep', 'tp'), may hold values from -0.125 to 0.125
Outputs:
- mixer_out: bfloat16 [65536, 2048], P(('grp', 'ep'), 'tp'), parts along dimension 0
- expert_out: bfloat16 [4096, 2048], P(('grp', 'ep'), 'tp'), parts along dimension 0
The draws below stay inside these ranges and needn't reach their ends.
There are 2 independent parts, one for each index of `grp`. The reference program is written for one: setup_inputs(seed, part) draws one part's arguments, and reference() takes and returns one part's arrays. A program takes and returns all parts, laid end to end along the dimension named above; an argument that names none is the same for every part. Nothing has to cross between parts.
Inputs may be any that keep to these rules, and one draw needn't show every extreme that they name: `routes`: A token's 2 experts differ. Among the 128 tokens of one index of ep, no expert is named more than 20 times, and in some of these blocks one is named exactly 20 times.
All inputs are finite; a program needn't handle non-finite values.
Results may differ from the reference program's by a relative error of at most 0.019.
Values may be sent and summed in bfloat16 or wider, within the bound.
No kernel may reach another device: no remote copies, remote signals or barrier semaphores. Data moves between devices by JAX's collectives and lax.ppermute only.
A program may use at most 64 MiB of HBM per device.

```python
import math
import jax
import jax.numpy as jnp
import numpy as np
from jax import lax

D = 2048
MEMORY_HEADS = 16
HEAD = 64
FF = 3584
BLK = 128
TOP = 2
SEG = 2048
ROWS = 128
SEQUENCE_TOKENS = 32768
TOKENS_B = 2048
EXPERTS = 16
CAP = 20
N_EP = 16
N_TP = 16


def draw_forget_gate(key, part):
    key_sequence = jax.random.split(jax.random.fold_in(key, 11), 5)
    chance = 0.5
    fast_head = jax.random.uniform(key_sequence[0], (MEMORY_HEADS,)) < chance
    base_rate = jnp.where(fast_head, 1.0 / 40.0, 0.25 / SEQUENCE_TOKENS)
    factor = jnp.exp(jax.random.uniform(key_sequence[1], (SEQUENCE_TOKENS // SEG, 1), minval=-0.7, maxval=0.7))
    factor = jnp.repeat(factor, SEG, axis=0)
    jitter = jnp.exp(0.5 * jnp.clip(jax.random.normal(key_sequence[2], (SEQUENCE_TOKENS, MEMORY_HEADS)), -3.0, 3.0))
    update_rate = base_rate[None, :] * factor * jitter
    surge_position = jax.random.randint(key_sequence[3], (2, MEMORY_HEADS), 0, SEQUENCE_TOKENS)
    token_position = jnp.arange(SEQUENCE_TOKENS)[:, None, None]
    surge_reached = jnp.any(token_position == surge_position[None], axis=1)
    surge_penalty = jax.random.uniform(key_sequence[4], (SEQUENCE_TOKENS, MEMORY_HEADS), minval=0.22, maxval=0.69)
    update_rate = jnp.where(surge_reached, surge_penalty, update_rate)
    return (-jnp.log(jnp.expm1(update_rate))).astype(jnp.float32)


def draw_input_gate(key, part):
    key_sequence = jax.random.split(jax.random.fold_in(key, 12), 1)
    gate_values = 1.5 * jnp.clip(jax.random.normal(key_sequence[0], (SEQUENCE_TOKENS, MEMORY_HEADS)), -4.0, 4.0)
    return gate_values.astype(jnp.float32)


def with_spikes(array, stream_key, source, target, blocks, factor):
    def block_of(position):
        return (jnp.arange(array.shape[position]) // (array.shape[position] // blocks)).reshape((-1,) + (1,) * (array.ndim - 1 - position))

    near = jax.random.permutation(stream_key, blocks)[block_of(target)]
    second = (block_of(target) + blocks // 2) % blocks
    return jnp.where((block_of(source) == near) | (block_of(source) == second), factor * array, array)


def shard_levels(own_key, shape, pieces, smallest, largest):
    def one(axis_at, parts):
        steps = jax.random.uniform(jax.random.fold_in(jax.random.fold_in(own_key, 6), axis_at), (parts,), jnp.float32, smallest / len(pieces), largest / len(pieces))
        return jnp.repeat(jnp.exp(steps), shape[axis_at] // parts).reshape((-1,) + (1,) * (len(shape) - axis_at - 1))

    loudness = one(*pieces[0])
    for cut in pieces[1:]:
        loudness = loudness * one(*cut)
    return loudness


def shared_out(rng, own, number, rows, count, top, most, skew):
    ranking = jax.random.permutation(rng, count)
    crowded, usual = shares(count, rows * top, most, skew, True), shares(count, rows * top, most, skew, False)
    places = jnp.arange(count)

    def named(lengths, rotation):
        used = int((lengths > 0).sum())
        fixed = max(1, used // 4)
        shifted = fixed + (places - fixed + rotation * (used - fixed)) % max(1, count - fixed)
        return jnp.zeros((count,), jnp.int32).at[ranking[jnp.where(places < fixed, places, shifted)]].set(jnp.asarray(lengths, jnp.int32))

    lengths = jnp.where(number % 4 == 0, named(crowded, number // 4), named(usual, number - number // 4 - 1))
    mixed = jax.random.permutation(jax.random.fold_in(own, 3), count)
    donor, sink = mixed[0:count // 2 * 2:2], mixed[1:count // 2 * 2:2]
    room = jnp.minimum(lengths[donor] - 1, most - lengths[sink]) // 2
    room = jnp.where((donor == ranking[0]) | (sink == ranking[0]) | (lengths[sink] == 0), 0, jnp.maximum(room, 0))
    shifted = jax.random.randint(jax.random.fold_in(own, 4), (count // 2,), 0, 1 << 20) % (room + 1)
    lengths = lengths.at[donor].add(-shifted).at[sink].add(shifted)
    items = jnp.searchsorted(jnp.cumsum(lengths), jnp.arange(rows * top), side="right").astype(jnp.int32)
    table = items.reshape(top, rows).T
    table = table[jax.random.permutation(jax.random.fold_in(own, 1), rows)]
    rotation = jax.random.randint(jax.random.fold_in(own, 2), (rows, 1), 0, top)
    return jnp.take_along_axis(table, (jnp.arange(top)[None, :] + rotation) % top, axis=1)


def shares(amount, total, limit, skew, full):
    loads = [(1 << 20) // math.isqrt(grade ** skew) + 1 for grade in range(1, amount + 1)]
    largest = limit if full else min(limit, max(-(-total // amount), total * loads[0] // sum(loads)))
    least = 1 if total - largest >= amount - 1 else 0
    given, rest = [largest] + [least] * (amount - 1), total - largest - least * (amount - 1)
    while rest > 0:
        free = [i for i in range(1, amount) if given[i] < largest] or [i for i in range(1, amount) if given[i] < limit]
        mass, remaining = sum([loads[i] for i in free]), rest
        for i in free:
            extra = min(limit - given[i], max(1, remaining * loads[i] // mass), rest)
            given[i] = given[i] + extra
            rest = rest - extra
    return np.array(given)


def bell_draw(key, extent, spread, most, shards=(), held_as=jnp.bfloat16):
    array = spread * jax.random.normal(key, extent, jnp.float32)
    if shards:
        array = array * shard_levels(key, extent, shards, -0.22, 0.18)
    return jnp.clip(array, -most, most).astype(held_as)


def bell_draw_with(stream_key, extent, width, reach, shards, heavy, kind=jnp.bfloat16):
    array = width * jax.random.normal(stream_key, extent, jnp.float32)
    if shards:
        array = array * shard_levels(stream_key, extent, shards, -0.22, 0.18)
    return jnp.clip(with_spikes(array, jax.random.fold_in(stream_key, 3), *heavy), -reach, reach).astype(kind)


def setup_inputs(seed: int = 0, part: int = 0) -> dict:
    arg_keys = jax.random.split(jax.random.key(seed), 15)
    part_keys = jax.random.split(jax.random.fold_in(arg_keys[14], part), 15)
    queries = bell_draw(part_keys[0], (SEQUENCE_TOKENS, MEMORY_HEADS * HEAD), 1.0, 6.0, ((0, 16), (1, 16)))
    key_vectors = bell_draw(part_keys[1], (SEQUENCE_TOKENS, MEMORY_HEADS * HEAD), 1.0, 6.0, ((0, 16), (1, 16)))
    value_vectors = bell_draw(part_keys[2], (SEQUENCE_TOKENS, MEMORY_HEADS * HEAD), 1.0, 6.0, ((0, 16), (1, 16)))
    input_gate = draw_input_gate(jax.random.fold_in(jax.random.fold_in(arg_keys[14], part), 71), part)
    forget_gate = draw_forget_gate(jax.random.fold_in(jax.random.fold_in(arg_keys[14], part), 71), part)
    head_gain = jnp.clip(1.0 + 0.18 * jax.random.normal(arg_keys[5], (MEMORY_HEADS * HEAD,), jnp.float32), 0.1, 1.9)
    out_weight = bell_draw(arg_keys[6], (MEMORY_HEADS * HEAD, D), (MEMORY_HEADS * HEAD) ** -0.5, 0.1875, ((1, 16),))
    expert_input = bell_draw(part_keys[7], (TOKENS_B, D), 1.0, 6.0, ((0, 16),))
    norm_gain = jnp.clip(1.0 + 0.18 * jax.random.normal(arg_keys[8], (D,), jnp.float32), 0.1, 1.9)
    routes_keys = jax.random.split(jax.random.fold_in(part_keys[9], 1), TOKENS_B // ROWS)
    routes_turns = jax.random.permutation(jax.random.fold_in(part_keys[9], 3), TOKENS_B // ROWS)
    routes = jax.vmap(lambda own, number: shared_out(jax.random.fold_in(part_keys[9], 2), own, number, ROWS, EXPERTS, TOP, CAP, 2))(routes_keys, routes_turns).reshape((TOKENS_B, TOP))
    route_weight = jnp.clip(0.25 + 0.75 * jax.random.uniform(part_keys[10], (TOKENS_B, TOP), jnp.float32) ** shard_levels(part_keys[10], (TOKENS_B, TOP), ((0, 16),), -0.2, 0.2), 0.25, 1.0)
    gate_weight = bell_draw(arg_keys[11], (EXPERTS, D, FF), D ** -0.5, 0.125, ((0, 16), (2, 16)))
    up_weight = bell_draw(arg_keys[12], (EXPERTS, D, FF), D ** -0.5, 0.125, ((0, 16), (2, 16)))
    down_weight = bell_draw_with(arg_keys[13], (EXPERTS, FF, D), FF ** -0.5, 0.125, ((0, 16), (1, 16)), (1, 2, 16, 2.0))
    return dict(queries=queries, key_vectors=key_vectors, value_vectors=value_vectors, input_gate=input_gate, forget_gate=forget_gate, head_gain=head_gain, out_weight=out_weight, expert_input=expert_input, norm_gain=norm_gain, routes=routes, route_weight=route_weight, gate_weight=gate_weight, up_weight=up_weight, down_weight=down_weight)


EXACT_PRECISION = lax.Precision.HIGHEST

def to_bfloat(values):
    return lax.optimization_barrier(values.astype(jnp.bfloat16)).astype(jnp.float32)

def head_blocks(matrix):
    return matrix.reshape(-1, BLK, MEMORY_HEADS, HEAD).transpose(2, 0, 1, 3).astype(jnp.float32)

def gate_blocks(matrix):
    return matrix.reshape(-1, BLK, MEMORY_HEADS).transpose(2, 0, 1)

def advance(carry, inputs):
    memory_matrix, normer_state, stable_state = carry
    block_end, tail_gate, key_block, block_values = inputs
    stable_next = jnp.maximum(block_end + stable_state, lax.optimization_barrier(jnp.max(tail_gate, axis=-1)))
    decay_factor = jnp.exp(block_end + stable_state - stable_next)
    key_weight = jnp.exp(tail_gate - stable_next[:, None])
    key_weighted_rows = to_bfloat(key_weight[..., None] * key_block)
    following_matrix = decay_factor[:, None, None] * memory_matrix + jnp.einsum('fjt,fjz->ftz', key_weighted_rows, block_values, precision=EXACT_PRECISION)
    normer_next = decay_factor[:, None] * normer_state + lax.optimization_barrier(jnp.sum(key_weighted_rows, axis=1))
    return ((following_matrix, normer_next, stable_next), (memory_matrix, normer_state, stable_state))

def head_cells(items):
    query_block, key_block, block_values, decay_sum, gate_in, matrix_in, normer_in, stable_in = items
    causal = jnp.arange(BLK)[:, None] >= jnp.arange(BLK)[None, :]
    log_weights = decay_sum[:, :, None] - decay_sum[:, None, :] + gate_in[:, None, :]
    log_weights = jnp.where(causal[None], log_weights, -jnp.inf)
    stabilizer = jnp.maximum(decay_sum + stable_in[:, None], lax.optimization_barrier(jnp.max(log_weights, axis=-1)))
    head_scale = HEAD ** (-0.5)
    scores = jnp.einsum('cjd,csd->cjs', query_block, key_block, precision=EXACT_PRECISION) * head_scale
    weighted = jnp.exp(log_weights - stabilizer[..., None]) * scores
    weighted_b = to_bfloat(weighted)
    carried_scale = jnp.exp(decay_sum + stable_in[:, None] - stabilizer)
    carried = jnp.einsum('cjk,ckv->cjv', query_block, matrix_in, precision=EXACT_PRECISION) * head_scale
    numerator = carried_scale[..., None] * carried + jnp.einsum('cjs,csv->cjv', weighted_b, block_values, precision=EXACT_PRECISION)
    denominator = carried_scale * jnp.einsum('cjk,ck->cj', query_block, normer_in, precision=EXACT_PRECISION) * head_scale + lax.optimization_barrier(jnp.sum(weighted, axis=-1))
    return numerator / jnp.maximum(jnp.abs(denominator), jnp.exp(-stabilizer))[..., None]

def expert_block(items):
    rows_in, gate_mat, up_mat, down_mat = items
    gate_act = jnp.dot(rows_in, gate_mat, preferred_element_type=jnp.float32)
    up_act = jnp.dot(rows_in, up_mat, preferred_element_type=jnp.float32)
    hidden = (jax.nn.silu(gate_act) * up_act).astype(jnp.bfloat16)
    group_width = FF // N_TP
    hidden_groups = hidden.reshape(-1, N_TP, group_width).astype(jnp.float32)
    down_groups = down_mat.reshape(N_TP, group_width, D).astype(jnp.float32)
    piece_sum = jnp.einsum('rgf,gfd->grd', hidden_groups, down_groups, precision=EXACT_PRECISION)
    piece_sum = to_bfloat(piece_sum)
    return lax.optimization_barrier(jnp.sum(piece_sum, axis=0)).astype(jnp.bfloat16)

def reference(queries, key_vectors, value_vectors, input_gate, forget_gate, head_gain, out_weight, expert_input, norm_gain, routes, route_weight, gate_weight, up_weight, down_weight):
    query_all = head_blocks(queries)
    key_all = head_blocks(key_vectors)
    value_all = head_blocks(value_vectors)
    gate_all = gate_blocks(input_gate)
    logf = gate_blocks(jax.nn.log_sigmoid(forget_gate))
    decay_sum = jnp.cumsum(logf, axis=-1)
    block_end = decay_sum[..., -1]
    tail_gate = block_end[..., None] - decay_sum + gate_all
    initial = (jnp.zeros((MEMORY_HEADS, HEAD, HEAD), jnp.float32), jnp.zeros((MEMORY_HEADS, HEAD), jnp.float32), jnp.zeros((MEMORY_HEADS,), jnp.float32))
    inputs = (jnp.moveaxis(block_end, 1, 0), jnp.moveaxis(tail_gate, 1, 0), jnp.moveaxis(key_all, 1, 0), jnp.moveaxis(value_all, 1, 0))
    ignored, entering = lax.scan(advance, initial, inputs)
    matrix_in, normer_in, stable_in = [jnp.moveaxis(part, 0, 1) for part in entering]
    cells = lax.map(head_cells, (query_all, key_all, value_all, decay_sum, gate_all, matrix_in, normer_in, stable_in))
    normed = cells * lax.rsqrt(lax.optimization_barrier(jnp.mean(cells * cells, axis=-1, keepdims=True)) + 1e-06)
    normed = (normed * head_gain.reshape(MEMORY_HEADS, 1, 1, HEAD)).astype(jnp.bfloat16)
    normed = normed.transpose(1, 2, 0, 3).reshape(-1, MEMORY_HEADS * HEAD)
    mixer_out = jnp.dot(normed, out_weight, preferred_element_type=jnp.float32).astype(jnp.bfloat16)
    input_wide = expert_input.astype(jnp.float32)
    scaled = input_wide * lax.rsqrt(lax.optimization_barrier(jnp.mean(input_wide * input_wide, axis=-1, keepdims=True)) + 1e-06)
    scaled = (scaled * norm_gain).astype(jnp.bfloat16)
    chosen = routes.reshape(N_EP, ROWS * TOP)
    onehot = (chosen[..., None] == jnp.arange(EXPERTS, dtype=jnp.int32)[None, None, :]).astype(jnp.int32)
    slot_index = lax.optimization_barrier(jnp.sum((jnp.cumsum(onehot, axis=1) - onehot) * onehot, axis=-1))
    block_index = jnp.arange(N_EP, dtype=jnp.int32)[:, None]
    target = (chosen * (N_EP * CAP) + block_index * CAP + slot_index).reshape(-1).astype(jnp.int32)
    source = jnp.repeat(jnp.arange(TOKENS_B, dtype=jnp.int32), TOP)
    buffer = jnp.zeros((EXPERTS * N_EP * CAP, D), jnp.bfloat16).at[target].set(scaled[source])
    buffer = buffer.reshape(EXPERTS, N_EP * CAP, D)
    results = lax.map(expert_block, (buffer, gate_weight, up_weight, down_weight)).reshape(-1, D)
    copies = results[target].astype(jnp.float32).reshape(TOKENS_B, TOP, D)
    expert_out = lax.optimization_barrier(jnp.sum(copies * route_weight[..., None], axis=1)).astype(jnp.bfloat16)
    return (mixer_out, expert_out)
```

```python
import functools

import jax
import jax.numpy as jnp
from jax import lax
from jax.experimental import pallas as pl
from jax.experimental.pallas import tpu as pltpu
from jax.sharding import Mesh
from jax.sharding import PartitionSpec as P

HEAD = 64
BLK = 128
TP = ("tp_0", "tp_1")
VERY_NEGATIVE = -1e30
AUG = 80
PAD = 24
PIECE = 56

F32 = jnp.float32
BF16 = jnp.bfloat16


def axis_index(name):
    return lax.axis_index(name)


def dot(left, right, left_dim, right_dim):
    return lax.dot_general(
        left, right, (((left_dim,), (right_dim,)), ((), ())), preferred_element_type=F32
    )


def split3(value):
    high = value.astype(BF16).astype(F32)
    middle = (value - high).astype(BF16).astype(F32)
    low = (value - high - middle).astype(BF16).astype(F32)
    return high, middle, low


def iota(shape, dim):
    return lax.broadcasted_iota(jnp.int32, shape, dim)


def slot_tables(routes, experts):
    choices, tokens = routes.shape
    expert = iota((experts, tokens), 0)
    named = [(expert == routes[k : k + 1, :]) for k in range(choices)]
    present = named[0]
    for other in named[1:]:
        present = present | other
    before = (iota((tokens, tokens), 0) < iota((tokens, tokens), 1)).astype(F32).astype(BF16)
    slot = dot(present.astype(F32).astype(BF16), before, 1, 0)
    slot_of_row = jnp.concatenate([iota((PAD, tokens), 0)] * experts, axis=0).astype(F32)

    def repeated(table):
        return jnp.concatenate(
            [jnp.broadcast_to(table[e : e + 1, :], (PAD, tokens)) for e in range(experts)], axis=0
        )

    hit = repeated(slot) == slot_of_row
    return [
        jnp.where(hit & (repeated(mask.astype(F32)) > 0.5), 1.0, 0.0).astype(F32) for mask in named
    ]


def first_kernel(q, k, v, gate_in, gate_forget, x, norm_gain, routes, pay, num_out, stat_out):
    segment = q.shape[1]
    blocks = segment // BLK
    head_scale = HEAD ** (-0.5)

    def blocked(ref):
        return jnp.concatenate(
            [ref[0:1, c * BLK : (c + 1) * BLK] for c in range(blocks)], axis=0
        )

    forget = blocked(gate_forget)
    gate = blocked(gate_in)
    small = jnp.exp(-jnp.abs(forget))
    one_more = 1.0 + small
    log1p = jnp.where(one_more == 1.0, small, jnp.log(one_more) * small / (one_more - 1.0 + 1e-38))
    logf = jnp.minimum(forget, 0.0) - log1p
    upper = iota((BLK, BLK), 0) <= iota((BLK, BLK), 1)
    ones_upper = upper.astype(F32).astype(BF16)
    decay = sum(dot(part.astype(BF16), ones_upper, 1, 0) for part in split3(logf))
    ends = decay[:, BLK - 1 : BLK]
    tail = ends - decay + gate
    peaks = jnp.max(tail, axis=1, keepdims=True)
    excess = gate - decay
    excess_columns = jnp.concatenate(
        [excess, jnp.zeros((BLK - blocks, BLK), F32)], axis=0
    ).T
    extra_rows = (iota((AUG - HEAD, BLK), 0) == 0).astype(F32).astype(BF16)

    state = jnp.zeros((AUG, HEAD), F32)
    stable = jnp.full((1, 1), VERY_NEGATIVE, F32)
    passed = jnp.zeros((1, 1), F32)
    for c in range(blocks):
        at = slice(c * BLK, (c + 1) * BLK)
        query, key, value = q[:, at], k[:, at], v[:, at]
        decay_row = decay[c : c + 1, :]
        log_weights = jnp.where(
            upper, excess_columns[:, c : c + 1] + decay_row, VERY_NEGATIVE
        )
        stabilizer = jnp.maximum(
            decay_row + stable, jnp.max(log_weights, axis=0, keepdims=True)
        )
        scores = dot(key, query, 0, 0) * head_scale
        weighted = jnp.exp(log_weights - stabilizer) * scores
        numerator = dot(value, weighted.astype(BF16), 1, 0)
        denominator = jnp.sum(weighted, axis=0, keepdims=True)
        if c:
            high = state.astype(BF16)
            low = (state - high.astype(F32)).astype(BF16)
            carried = dot(high, query, 1, 0) + dot(low, query, 1, 0)
            scale = jnp.exp(decay_row + stable - stabilizer) * head_scale
            numerator = numerator + scale * carried[:HEAD]
            denominator = denominator + scale * carried[HEAD : HEAD + 1]
        num_out[:, at] = numerator
        stat_out[0:1, at] = denominator
        stat_out[1:2, at] = stabilizer
        stat_out[2:3, at] = passed + decay_row
        end = ends[c : c + 1, :]
        following = jnp.maximum(end + stable, peaks[c : c + 1, :])
        key_weight = jnp.exp(tail[c : c + 1, :] - following)
        weighted_keys = (key_weight * key.astype(F32)).astype(BF16)
        update = dot(jnp.concatenate([value, extra_rows], axis=0), weighted_keys, 1, 1)
        state = jnp.exp(end + stable - following) * state + update
        stable = following
        passed = passed + end

    experts = pay.shape[0]
    index = axis_index("tp_0") * lax.axis_size("tp_1") + axis_index("tp_1")
    at = pl.multiple_of(index * BLK, BLK)
    wide = x[...].astype(F32)
    mean = jnp.mean(wide * wide, axis=1, keepdims=True)
    narrow = x[:, pl.ds(at, BLK)].astype(F32) * lax.rsqrt(mean + 1e-06)
    narrow = (narrow * norm_gain[0:1, pl.ds(at, BLK)]).astype(BF16)
    tables = slot_tables(routes[...], experts)
    table = tables[0]
    for other in tables[1:]:
        table = table + other
    slots = dot(table.astype(BF16), narrow, 1, 0)

    lane = iota((1, HEAD), 1)
    scalars = jnp.zeros((1, HEAD), F32)
    for j, part in enumerate(split3(passed) + split3(stable)):
        scalars = jnp.where(lane == j, part, scalars)
    line = jnp.concatenate([state[HEAD : HEAD + 1, :], scalars], axis=1)
    half = HEAD // 2
    packed = jnp.concatenate([state[:half, :], state[half:HEAD, :]], axis=1)
    line_row = iota((PAD, BLK), 0) == PAD - 4
    for e in range(experts):
        rows = jnp.where(line_row, line, slots[e * PAD : (e + 1) * PAD, :])
        pay[e] = jnp.concatenate([rows, packed], axis=0).astype(BF16)


def second_kernel(got, q, num, stat, gain, normed, rows_out, rows):
    peers = got.shape[0]
    segment = q.shape[1]
    head_scale = HEAD ** (-0.5)
    mine = axis_index("ep")
    capacity = rows.shape[0] // peers

    for e in range(peers):
        rows[e * capacity : (e + 1) * capacity, :] = got[e][:capacity].astype(F32)
    packed_rows = rows[...].astype(BF16)
    for i in range(rows_out.shape[0]):
        rows_out[i] = packed_rows

    lines = [got[e, 16:32, :].astype(F32)[PAD - 20 : PAD - 19, :] for e in range(peers)]
    decays = [sum(line[:, HEAD + j : HEAD + j + 1] for j in range(3)) for line in lines]
    levels = [sum(line[:, HEAD + j : HEAD + j + 1] for j in range(3, 6)) for line in lines]
    later = jnp.zeros((1, 1), F32)
    logs = [None] * peers
    for e in reversed(range(peers)):
        earlier = e < mine
        logs[e] = jnp.where(earlier, levels[e] + later, VERY_NEGATIVE)
        later = later + jnp.where(earlier, decays[e], 0.0)
    level = later
    for e in range(peers):
        level = jnp.maximum(level, logs[e])
    half = HEAD // 2
    packed = jnp.zeros((half, BLK), F32)
    line = jnp.zeros((1, BLK), F32)
    for e in range(peers):
        weight = jnp.exp(logs[e] - level)
        packed = packed + weight * got[e].astype(F32)[PAD:PIECE, :]
        line = line + weight * lines[e]
    state = jnp.concatenate(
        [
            packed[:, :HEAD],
            packed[:, HEAD:],
            jnp.where(iota((AUG - HEAD, HEAD), 0) == 0, line[:, :HEAD], 0.0),
        ],
        axis=0,
    )
    high = state.astype(BF16)
    low = (state - high.astype(F32)).astype(BF16)
    square = iota((HEAD, HEAD), 0) == iota((HEAD, HEAD), 1)
    gain_column = jnp.sum(
        jnp.where(square, jnp.broadcast_to(gain[...], (HEAD, HEAD)), 0.0), axis=1, keepdims=True
    )
    width = 2 * BLK
    for c in range(segment // width):
        at = slice(c * width, (c + 1) * width)
        query = q[:, at]
        carried = dot(high, query, 1, 0) + dot(low, query, 1, 0)
        local = stat[1:2, at]
        entering = stat[2:3, at] + level
        stabilizer = jnp.maximum(entering, local)
        scale = jnp.exp(entering - stabilizer) * head_scale
        keep = jnp.exp(local - stabilizer)
        numerator = keep * num[:, at] + scale * carried[:HEAD]
        denominator = keep * stat[0:1, at] + scale * carried[HEAD : HEAD + 1]
        cells = numerator * (1.0 / jnp.maximum(jnp.abs(denominator), jnp.exp(-stabilizer)))
        mean = jnp.mean(cells * cells, axis=0, keepdims=True)
        normed[:, at] = (cells * lax.rsqrt(mean + 1e-06) * gain_column).astype(BF16)


def expert_kernel(own, other, gate, up, down, keep, send):
    slices = own.shape[0]
    width = 2 * BLK
    first = axis_index("tp_1") == 0
    gate_act = None
    for s in range(slices):
        a, b = own[s], other[s]
        left = jnp.concatenate([jnp.where(first, a, b), jnp.where(first, b, a)], axis=1)
        at = slice(s * width, (s + 1) * width)
        gate_part = dot(left, gate[:, at], 1, 1)
        up_part = dot(left, up[:, at], 1, 1)
        gate_act = gate_part if gate_act is None else gate_act + gate_part
        up_act = up_part if s == 0 else up_act + up_part
    hidden = (gate_act / (1.0 + jnp.exp(-gate_act)) * up_act).astype(BF16)
    for s in range(slices):
        piece = dot(hidden, down[:, s * width : (s + 1) * width], 1, 0)
        a, b = piece[:, :BLK], piece[:, BLK:]
        keep[s] = jnp.where(first, a, b).astype(BF16)
        send[s] = jnp.where(first, b, a).astype(BF16)


def sum_kernel(parts, out, rows):
    total = parts[0].astype(F32)
    for s in range(1, parts.shape[0]):
        total = total + parts[s].astype(F32)
    rows[...] = total
    experts, capacity, _ = out.shape
    for e in range(experts):
        out[e] = rows[e * capacity : (e + 1) * capacity, :].astype(BF16)


def last_kernel(got, routes, weight, out):
    experts, capacity, width = got.shape
    tables = slot_tables(routes[...], experts)
    table = None
    for k, one in enumerate(tables):
        part = one * weight[k : k + 1, :]
        table = part if table is None else table + part
    high = table.astype(BF16)
    low = (table - high.astype(F32)).astype(BF16)
    padding = jnp.zeros((PAD - capacity, width), F32)
    pieces = []
    for e in range(experts):
        pieces += [got[e].astype(F32), padding]
    values = jnp.concatenate(pieces, axis=0).astype(BF16)
    out[...] = (dot(high, values, 0, 0) + dot(low, values, 0, 0)).astype(BF16)


def call(kernel, outs, *args, scratch=()):
    return pl.pallas_call(
        kernel,
        out_shape=tuple(jax.ShapeDtypeStruct(*one) for one in outs),
        scratch_shapes=list(scratch),
    )(*args)


def on_device(
    queries,
    key_vectors,
    value_vectors,
    input_gate,
    forget_gate,
    head_gain,
    out_weight,
    expert_input,
    norm_gain,
    routes,
    route_weight,
    gate_weight,
    up_weight,
    down_weight,
):
    segment = queries.shape[0]
    tokens, features = expert_input.shape
    experts = lax.axis_size("ep")
    slices = lax.axis_size("tp_0")
    capacity = 5 * tokens * routes.shape[1] // (4 * experts)
    slots = experts * capacity
    routes_rows = routes.T
    pay, num, stat = call(
        first_kernel,
        [
            ((experts, PIECE, BLK), BF16),
            ((HEAD, segment), F32),
            ((8, segment), F32),
        ],
        queries.T,
        key_vectors.T,
        value_vectors.T,
        input_gate.T,
        forget_gate.T,
        expert_input,
        norm_gain.reshape(1, features),
        routes_rows,
    )
    got = lax.all_to_all(pay, "ep", 0, 0, tiled=True)
    normed, rows = call(
        second_kernel,
        [((HEAD, segment), BF16), ((slices, slots, BLK), BF16)],
        got,
        queries.T,
        num,
        stat,
        head_gain.reshape(1, HEAD),
        scratch=[pltpu.VMEM((slots, BLK), F32)],
    )
    all_normed = lax.all_gather(normed, TP, axis=0, tiled=True)
    swap = [(0, 1), (1, 0)]
    own = lax.all_to_all(rows, "tp_0", 0, 0, tiled=True)
    other = lax.ppermute(own, "tp_1", swap)
    keep, send = call(
        expert_kernel,
        [((slices, slots, BLK), BF16)] * 2,
        own,
        other,
        gate_weight[0].T,
        up_weight[0].T,
        down_weight[0],
    )
    pair = (keep.astype(F32) + lax.ppermute(send, "tp_1", swap).astype(F32)).astype(BF16)
    parts = lax.all_to_all(pair, "tp_0", 0, 0, tiled=True)
    (summed,) = call(
        sum_kernel,
        [((experts, capacity, BLK), BF16)],
        parts,
        scratch=[pltpu.VMEM((slots, BLK), F32)],
    )
    returned = lax.all_to_all(summed, "ep", 0, 0, tiled=True)
    (expert_out,) = call(
        last_kernel, [((tokens, BLK), BF16)], returned, routes_rows, route_weight.T
    )
    mixer_out = dot(all_normed, out_weight, 0, 0).astype(BF16)
    return (mixer_out, expert_out)


def solution(mesh):
    chips = mesh.shape["tp"] // 2
    torus = Mesh(
        mesh.devices.reshape(mesh.shape["grp"], mesh.shape["ep"], chips, 2),
        ("grp", "ep", "tp_0", "tp_1"),
    )
    in_specs = (
        P(("grp", "ep"), TP),
        P(("grp", "ep"), TP),
        P(("grp", "ep"), TP),
        P(("grp", "ep"), TP),
        P(("grp", "ep"), TP),
        P(TP),
        P(None, TP),
        P(("grp", "ep"), None),
        P(),
        P(("grp", "ep"), None),
        P(("grp", "ep"), None),
        P("ep", None, TP),
        P("ep", None, TP),
        P("ep", TP, None),
    )
    out_specs = (P(("grp", "ep"), TP), P(("grp", "ep"), TP))
    return jax.shard_map(
        on_device, mesh=torus, in_specs=in_specs, out_specs=out_specs, check_vma=False
    )
```
